32 devices in a mesh: grp: 2 (over y), sp: 4 (over z), tp: 4 (over x, core).
Axes of the slice: x: 2, y: 2, z: 4, core: 2. Of those that a mesh axis runs over, the one named last changes fastest.
Arguments:
- latent: bfloat16 [4096, 4096], P(('grp', 'sp'), 'tp'), parts along dimension 0, may hold values from -42 to 42
- context: bfloat16 [2048, 4096], P(('grp', 'sp'), 'tp'), parts along dimension 0, may hold values from -42 to 42
- conditions: float32 [4, 4096], P('grp', 'sp'), parts along dimension 0, may hold values from -6 to 6
- mod_weight: bfloat16 [4096, 3, 4096], P('sp', None, 'tp'), may hold values from -0.09375 to 0.09375
- norm_gain: float32 [4096], P('tp'), may hold values from 0.1 to 1.9
- w_query: bfloat16 [4096, 2048], P(None, 'tp'), may hold values from -0.09375 to 0.09375
- w_key: bfloat16 [4096, 2048], P(None, 'tp'), may hold values from -0.09375 to 0.09375
- w_value: bfloat16 [4096, 2048], P(None, 'tp'), may hold values from -0.09375 to 0.09375
- query_gain: float32 [64], replicated, may hold values from 1 to 14
- key_gain: float32 [64], replicated, may hold values from 1 to 14
- lambdas: float32 [16], P('tp'), may hold values from 0.3 to 0.8
- out_gain: float32 [128], replicated, may hold values from 0.1 to 1.9
- w_out: bfloat16 [2048, 4096], P(None, 'tp'), may hold values from -0.125 to 0.125
Outputs:
- updated: bfloat16 [4096, 4096], P(('grp', 'sp'), 'tp'), parts along dimension 0
The draws below stay inside these ranges and needn't reach their ends.
There are 2 independent parts, one for each index of `grp`. The reference program is written for one: setup_inputs(seed, part) draws one part's arguments, and reference() takes and returns one part's arrays. A program takes and returns all parts, laid end to end along the dimension named above; an argument that names none is the same for every part. Nothing has to cross between parts.
All inputs are finite; a program needn't handle non-finite values.
Results may differ from the reference program's by a relative error of at most 0.0076.
Values may be sent and summed in bfloat16 or wider, within the bound.
No kernel may reach another device: no remote copies, remote signals or barrier semaphores. Data moves between devices by JAX's collectives and lax.ppermute only.
A program may use at most 128 MiB of HBM per device.

```python
import math
import jax
import jax.numpy as jnp
from jax import lax

D = 4096
HEADS = 16
DK = 64
DV = 128
GRID_W = 64
CTX = 1024
LAT = 2048


def rising_rows(key, row_count):
    column = jnp.arange(D, dtype=jnp.float32)
    base = jnp.clip(jax.random.normal(key, (row_count, D), jnp.float32), -6.0, 6.0)
    return base * (1.0 + 2.0 * column / (D - 1))


def spiked_gains(key, which):
    own_key = jax.random.fold_in(key, which)
    return jax.random.uniform(own_key, (DK,), jnp.float32, 1.1, 1.5)


def draw_latent(key, part):
    return rising_rows(jax.random.fold_in(key, 21), LAT).astype(jnp.bfloat16)


def draw_context(key, part):
    return rising_rows(jax.random.fold_in(key, 22), CTX).astype(jnp.bfloat16)


def draw_query_gain(key, part):
    return spiked_gains(key, 1)


def draw_key_gain(key, part):
    return spiked_gains(key, 2)


def shard_levels(key, extent, pieces, smallest, high):
    loudness = 1.0
    for dim, parts in pieces:
        heights = jax.random.uniform(jax.random.fold_in(jax.random.fold_in(key, 6), dim), (parts,), jnp.float32, smallest / len(pieces), high / len(pieces))
        loudness = loudness * jnp.repeat(jnp.exp(heights), extent[dim] // parts).reshape((-1,) + (1,) * (len(extent) - 1 - dim))
    return loudness


def bell_draw(key, dims, deviation, most, shards=(), kind=jnp.bfloat16):
    result = deviation * jax.random.normal(key, dims, jnp.float32)
    if shards:
        result = result * shard_levels(key, dims, shards, -0.22, 0.18)
    return jnp.clip(result, -most, most).astype(kind)


def setup_inputs(seed: int = 0, part: int = 0) -> dict:
    keys = jax.random.split(jax.random.key(seed), 14)
    own_keys = jax.random.split(jax.random.fold_in(keys[13], part), 14)
    latent = draw_latent(jax.random.fold_in(jax.random.fold_in(keys[13], part), 71), part)
    context = draw_context(jax.random.fold_in(jax.random.fold_in(keys[13], part), 71), part)
    conditions = bell_draw(own_keys[2], (2, D), 1.0, 6.0, ((1, 4),), jnp.float32)
    mod_weight = bell_draw(keys[3], (D, 3, D), D ** -0.5, 0.09375, ((0, 4), (2, 4)))
    norm_gain = jnp.clip(1.0 + 0.18 * jax.random.normal(keys[4], (D,), jnp.float32), 0.1, 1.9)
    w_query = bell_draw(keys[5], (D, HEADS * 2 * DK), D ** -0.5, 0.09375, ((1, 4),))
    w_key = bell_draw(keys[6], (D, HEADS * 2 * DK), D ** -0.5, 0.09375, ((1, 4),))
    w_value = bell_draw(keys[7], (D, HEADS * DV), D ** -0.5, 0.09375, ((1, 4),))
    query_gain = draw_query_gain(jax.random.fold_in(keys[13], 71), part)
    key_gain = draw_key_gain(jax.random.fold_in(keys[13], 71), part)
    lambdas = jnp.clip(0.3 + 0.5 * jax.random.uniform(keys[10], (HEADS,), jnp.float32) ** shard_levels(keys[10], (HEADS,), ((0, 4),), -0.2, 0.2), 0.3, 0.8)
    out_gain = jnp.clip(1.0 + 0.18 * jax.random.normal(keys[11], (DV,), jnp.float32), 0.1, 1.9)
    w_out = bell_draw(keys[12], (HEADS * DV, D), (HEADS * DV) ** -0.5, 0.125, ((1, 4),))
    return {"latent": latent, "context": context, "conditions": conditions, "mod_weight": mod_weight, "norm_gain": norm_gain, "w_query": w_query, "w_key": w_key, "w_value": w_value, "query_gain": query_gain, "key_gain": key_gain, "lambdas": lambdas, "out_gain": out_gain, "w_out": w_out}


epsilon = 1e-06

def turn_half(halves, angles):
    quarter = halves.shape[-1] // 2
    cosine = jnp.cos(angles)[:, None, None, :]
    sine_part = jnp.sin(angles)[:, None, None, :]
    first_part = halves[..., :quarter]
    second = halves[..., quarter:]
    return jnp.concatenate([first_part * cosine - second * sine_part, first_part * sine_part + second * cosine], axis=-1)

def rotate(features, positions):
    half_width = features.shape[-1] // 2
    quarter = half_width // 2
    inverse = 10000.0 ** (-2.0 * jnp.arange(quarter, dtype=jnp.float32) / half_width)
    grid_row = (positions // GRID_W).astype(jnp.float32)
    grid_column = (positions % GRID_W).astype(jnp.float32)
    return jnp.concatenate([turn_half(features[..., :half_width], grid_row[:, None] * inverse), turn_half(features[..., half_width:], grid_column[:, None] * inverse)], axis=-1)

def head_norm(features, gain_row):
    return features * lax.rsqrt(lax.optimization_barrier(jnp.mean(features * features, axis=-1, keepdims=True)) + epsilon) * gain_row

def modulate(rows_in, gain_row, shift_row, scale_row):
    floats = rows_in.astype(jnp.float32)
    factor = lax.rsqrt(lax.optimization_barrier(jnp.mean(floats * floats, axis=1, keepdims=True)) + epsilon)
    return (floats * factor * gain_row * (1.0 + scale_row) + shift_row).astype(jnp.bfloat16)

def reference(latent, context, conditions, mod_weight, norm_gain, w_query, w_key, w_value, query_gain, key_gain, lambdas, out_gain, w_out):
    activated = jax.nn.silu(conditions).astype(jnp.bfloat16)
    modulation = jnp.dot(activated, mod_weight.reshape(D, 3 * D), preferred_element_type=jnp.float32).reshape(2, 3, D)
    hidden = modulate(latent, norm_gain, modulation[0, 0], modulation[0, 1])
    hidden_ctx = modulate(context, norm_gain, modulation[1, 0], modulation[1, 1])
    positions = jnp.arange(LAT, dtype=jnp.int32)
    query_raw = jnp.dot(hidden, w_query, preferred_element_type=jnp.float32).reshape(LAT, HEADS, 2, DK)
    key_raw = jnp.dot(hidden, w_key, preferred_element_type=jnp.float32).reshape(LAT, HEADS, 2, DK)
    ctx_key_raw = jnp.dot(hidden_ctx, w_key, preferred_element_type=jnp.float32).reshape(CTX, HEADS, 2, DK)
    queries = rotate(head_norm(query_raw, query_gain), positions).astype(jnp.bfloat16)
    lat_keys = rotate(head_norm(key_raw, key_gain), positions).astype(jnp.bfloat16)
    ctx_keys = head_norm(ctx_key_raw, key_gain).astype(jnp.bfloat16)
    lat_values = jnp.dot(hidden, w_value, preferred_element_type=jnp.float32).astype(jnp.bfloat16).reshape(LAT, HEADS, DV)
    ctx_values = jnp.dot(hidden_ctx, w_value, preferred_element_type=jnp.float32).astype(jnp.bfloat16).reshape(CTX, HEADS, DV)
    all_keys = jnp.concatenate([ctx_keys, lat_keys], axis=0)
    all_values = jnp.concatenate([ctx_values, lat_values], axis=0)
    block_rows = math.gcd(LAT, 512)
    scaling = DK ** (-0.5)

    def one_head(head_index):
        head_keys = lax.dynamic_index_in_dim(all_keys, head_index, 1, False).astype(jnp.float32)
        head_values = lax.dynamic_index_in_dim(all_values, head_index, 1, False).astype(jnp.float32)
        head_queries = lax.dynamic_index_in_dim(queries, head_index, 1, False).astype(jnp.float32)
        head_queries = head_queries.reshape(LAT // block_rows, block_rows, 2, DK)
        weight_lambda = lax.dynamic_index_in_dim(lambdas, head_index, 0, False)

        def one_block(query_block):
            scores = jnp.einsum('qmd,kmd->qmk', query_block, head_keys) * scaling
            row_peak = lax.optimization_barrier(jnp.max(scores, axis=-1, keepdims=True))
            exponent = jnp.exp(scores - row_peak)
            row_sums = lax.optimization_barrier(jnp.sum(exponent, axis=-1))
            weights = lax.optimization_barrier(exponent.astype(jnp.bfloat16)).astype(jnp.float32)
            blended = jnp.einsum('qmk,kv->qmv', weights, head_values)
            attended = blended[:, 0] / row_sums[:, 0, None] - weight_lambda * blended[:, 1] / row_sums[:, 1, None]
            return head_norm(attended, out_gain)
        return lax.map(one_block, head_queries).reshape(LAT, DV)
    outputs = lax.map(one_head, jnp.arange(HEADS, dtype=jnp.int32))
    head_out = jnp.transpose(outputs, (1, 0, 2)).reshape(LAT, HEADS * DV).astype(jnp.bfloat16)
    mixed_rows = jnp.dot(head_out, w_out, preferred_element_type=jnp.float32)
    return (latent.astype(jnp.float32) + modulation[0, 2] * mixed_rows).astype(jnp.bfloat16)
```

```python
import functools

import jax
import jax.numpy as jnp
from jax import lax
from jax.experimental import pallas as pl
from jax.experimental.pallas import tpu as pltpu
from jax.sharding import PartitionSpec as P

GRID_W = 64
EPS = 1e-06
F32 = jnp.float32
BF16 = jnp.bfloat16
VMEM_LIMIT = 60 * 1024 * 1024


def tables(positions, dk):
    half, quarter = dk // 2, dk // 4
    lane = jnp.arange(2 * dk, dtype=jnp.int32) % dk
    inverse = 10000.0 ** (-2.0 * (lane % quarter).astype(F32) / half)
    grid_row = (positions // GRID_W).astype(F32)[:, None]
    grid_column = (positions % GRID_W).astype(F32)[:, None]
    angles = jnp.where(lane[None] < half, grid_row, grid_column) * inverse[None]
    sign = jnp.where(lane % half < quarter, -1.0, 1.0).astype(F32)
    return jnp.cos(angles), jnp.sin(angles) * sign[None]


def project_kernel(order, my_ref, other_ref, mods_ref, *refs, parts, weights, turned, features):
    w_refs = [refs[i * parts : (i + 1) * parts] for i in range(weights)]
    refs = refs[weights * parts :]
    gain_refs, refs = refs[: weights - 1], refs[weights - 1 :]
    if turned:
        cos_ref, sin_ref = refs[:2]
        refs = refs[2:]
    out_ref, hidden = refs
    half_parts = parts // 2

    @pl.when(pl.program_id(0) == 0)
    def _():
        total = None
        for b in range(parts):
            src = my_ref if b < half_parts else other_ref
            rows = src[b % half_parts].astype(F32)
            part = jnp.sum(rows * rows, axis=-1, keepdims=True)
            total = part if total is None else total + part
        factor = lax.rsqrt(total / features + EPS)
        for b in range(parts):
            src = my_ref if b < half_parts else other_ref
            rows = src[b % half_parts].astype(F32)
            gain = mods_ref[b, 0:1, :] * (1.0 + mods_ref[b, 1:2, :])
            hidden[b] = (rows * factor * gain + mods_ref[b, 2:3, :]).astype(BF16)

    def product(w):
        total = None
        for b in range(parts):
            part = jnp.dot(hidden[b], w_refs[w][b][...], preferred_element_type=F32)
            total = part if total is None else total + part
        return total

    heads, rows, width = out_ref.shape
    dv = width // weights
    dk = dv // 2
    lane = lax.broadcasted_iota(jnp.int32, (rows, dv), 1)
    low = lane < dk
    first = lane % (dk // 2) < dk // 4
    for w in range(weights):
        raw = product(w)
        for h in range(heads):
            v = raw[:, h * dv : (h + 1) * dv]
            if w < weights - 1:
                sq = v * v
                low_sum = jnp.sum(jnp.where(low, sq, 0.0), axis=-1, keepdims=True)
                high_sum = jnp.sum(jnp.where(low, 0.0, sq), axis=-1, keepdims=True)
                mean = jnp.where(low, low_sum, high_sum) / dk
                v = v * lax.rsqrt(mean + EPS) * gain_refs[w][...]
                if turned:
                    swapped = jnp.where(
                        first, pltpu.roll(v, dv - dk // 4, 1), pltpu.roll(v, dk // 4, 1)
                    )
                    v = v * cos_ref[...] + swapped * sin_ref[...]
            out_ref[h, :, w * dv : (w + 1) * dv] = v.astype(BF16)


def project(order, my, other, mods, w_list, gains, cos_sin, dv):
    half_parts, rows, width = my.shape
    parts = 2 * half_parts
    cols = w_list[0].shape[1]
    block = min(cols, 2 * dv)
    weights = len(w_list)
    full = lambda shape: pl.BlockSpec(shape, lambda j, order: (0,) * len(shape))
    in_specs = [full(my.shape), full(other.shape), full(mods.shape)]
    operands = [my, other, mods]
    for w in w_list:
        for b in range(parts):
            in_specs.append(pl.BlockSpec((width, block), lambda j, order, b=b: (order[b], j)))
            operands.append(w)
    for extra in list(gains) + list(cos_sin):
        in_specs.append(full(extra.shape))
        operands.append(extra)
    return pl.pallas_call(
        functools.partial(
            project_kernel,
            parts=parts,
            weights=weights,
            turned=bool(cos_sin),
            features=float(parts * width),
        ),
        grid_spec=pltpu.PrefetchScalarGridSpec(
            num_scalar_prefetch=1,
            grid=(cols // block,),
            in_specs=in_specs,
            out_specs=pl.BlockSpec((block // dv, rows, weights * dv), lambda j, order: (j, 0, 0)),
            scratch_shapes=[pltpu.VMEM((parts, rows, width), BF16)],
        ),
        out_shape=jax.ShapeDtypeStruct((cols // dv, rows, weights * dv), BF16),
        compiler_params=pltpu.CompilerParams(vmem_limit_bytes=VMEM_LIMIT),
        cost_estimate=pl.CostEstimate(
            flops=2 * rows * parts * width * cols * weights,
            transcendentals=0,
            bytes_accessed=2 * parts * width * cols * weights,
        ),
    )(order, *operands)


def attend_kernel(lam_ref, *refs, scaling, step, pairs, resumed, final, after):
    q_ref, refs = refs[0], refs[1:]
    key_refs, refs = [refs[2 * i : 2 * i + 2] for i in range(pairs)], refs[2 * pairs :]
    gain_ref, refs = refs[0], refs[1:]
    if resumed:
        old_refs, refs = refs[:3], refs[3:]
    outs = refs[after:]
    q = q_ref[0]
    rows, dv = q.shape
    lane = lax.broadcasted_iota(jnp.int32, (rows, dv), 1)
    zero = jnp.zeros_like(q)
    both = jnp.concatenate(
        [jnp.where(lane < dv // 2, q, zero), jnp.where(lane < dv // 2, zero, q)], axis=0
    )
    pieces = []
    for k_ref, v_ref in key_refs:
        count = k_ref.shape[1]
        size = min(count, step)
        pieces += [(k_ref, v_ref, start, size) for start in range(0, count, size)]

    def fold(x, combine, whole, so_far):
        for c in range(0, x.shape[1], 128):
            part = x[:, c : c + 128]
            if part.shape[1] < 128:
                part = jnp.pad(part, ((0, 0), (0, 128 - part.shape[1])), constant_values=whole)
            so_far = part if so_far is None else combine(so_far, part)
        return so_far

    scores = []
    peak = None
    for k_ref, _, start, size in pieces:
        s = lax.dot_general(
            both, k_ref[0, start : start + size, :], (((1,), (1,)), ((), ())),
            preferred_element_type=F32,
        )
        scores.append(s)
        peak = fold(s, jnp.maximum, -jnp.inf, peak)
    factor = scaling * 1.4426950408889634
    peak = jnp.max(peak, axis=-1, keepdims=True) * factor
    if resumed:
        old_peak = old_refs[1][0][:, :1]
        peak = jnp.maximum(peak, old_peak)
    sums = None
    blended = None
    for (_, v_ref, start, size), s in zip(pieces, scores):
        expo = jnp.exp2(s * factor - peak)
        sums = fold(expo, jnp.add, 0.0, sums)
        more = jnp.dot(
            expo.astype(BF16), v_ref[0, start : start + size, :], preferred_element_type=F32
        )
        blended = more if blended is None else blended + more
    sums = jnp.sum(sums, axis=-1, keepdims=True)
    if resumed:
        shrink = jnp.exp2(old_peak - peak)
        blended = blended + old_refs[0][0] * shrink
        sums = sums + old_refs[2][0][:, :1] * shrink
    if not final:
        outs[0][0] = blended
        outs[1][0] = jnp.broadcast_to(peak, (2 * rows, 128))
        outs[2][0] = jnp.broadcast_to(sums, (2 * rows, 128))
        return
    normed = blended / sums
    attended = normed[:rows] - lam_ref[pl.program_id(0)] * normed[rows:]
    mean = jnp.mean(attended * attended, axis=-1, keepdims=True)
    outs[0][0] = (attended * lax.rsqrt(mean + EPS) * gain_ref[...]).astype(BF16)


def attend(lam, q, q_at, keys, gain, dv, state=(), final=True, after=(), share=(0, 1)):
    heads, count = q.shape[0], q.shape[1] // share[1]
    total = sum(x.shape[1] for x, _ in keys)
    rows = min(count, 256 if total <= 4096 else 128)
    first = share[0] * (count // rows)
    spec = lambda n, at: pl.BlockSpec((1, n, dv), lambda h, i: (h, 0, at))
    kept = lambda width: pl.BlockSpec((1, 2 * rows, width), lambda h, i: (h, i, 0))
    in_specs = [
        pl.BlockSpec(memory_space=pltpu.SMEM),
        pl.BlockSpec((1, rows, dv), lambda h, i: (h, first + i, q_at)),
    ]
    operands = [lam, q]
    for x, at in keys:
        in_specs += [spec(x.shape[1], at), spec(x.shape[1], at + 1)]
        operands += [x, x]
    in_specs.append(pl.BlockSpec((1, dv), lambda h, i: (0, 0)))
    operands.append(gain)
    for x in state:
        in_specs.append(kept(x.shape[2]))
        operands.append(x)
    for x in after:
        in_specs.append(pl.BlockSpec(memory_space=pl.ANY))
        operands.append(x)
    if final:
        out_specs = pl.BlockSpec((1, rows, dv), lambda h, i: (h, i, 0))
        out_shape = jax.ShapeDtypeStruct((heads, count, dv), BF16)
    else:
        out_specs = [kept(dv), kept(128), kept(128)]
        out_shape = [
            jax.ShapeDtypeStruct((heads, 2 * count, width), F32) for width in (dv, 128, 128)
        ]
    return pl.pallas_call(
        functools.partial(
            attend_kernel, scaling=(dv // 2) ** -0.5, step=512, pairs=len(keys),
            resumed=bool(state), final=final, after=len(after),
        ),
        grid=(heads, count // rows),
        in_specs=in_specs,
        out_specs=out_specs,
        out_shape=out_shape,
        compiler_params=pltpu.CompilerParams(vmem_limit_bytes=VMEM_LIMIT),
        cost_estimate=pl.CostEstimate(
            flops=12 * heads * count * total * dv,
            transcendentals=2 * heads * count * total,
            bytes_accessed=4 * heads * total * dv,
        ),
    )(*operands)


def mix_kernel(order, my_ref, other_ref, lat_ref, gate_ref, *refs, parts):
    out_ref = refs[parts]
    half_parts = parts // 2
    total = None
    for b in range(parts):
        src = my_ref if b < half_parts else other_ref
        part = jnp.dot(src[b % half_parts], refs[b][...], preferred_element_type=F32)
        total = part if total is None else total + part
    out_ref[...] = (lat_ref[...].astype(F32) + gate_ref[...] * total).astype(BF16)


def mix(order, my, other, latent, gate, w_out):
    half_parts, rows, width = my.shape
    parts = 2 * half_parts
    cols = w_out.shape[1]
    block = min(cols, 256)
    full = lambda shape: pl.BlockSpec(shape, lambda j, order: (0,) * len(shape))
    return pl.pallas_call(
        functools.partial(mix_kernel, parts=parts),
        grid_spec=pltpu.PrefetchScalarGridSpec(
            num_scalar_prefetch=1,
            grid=(cols // block,),
            in_specs=[
                full(my.shape),
                full(other.shape),
                pl.BlockSpec((rows, block), lambda j, order: (0, j)),
                pl.BlockSpec((1, block), lambda j, order: (0, j)),
            ]
            + [
                pl.BlockSpec((width, block), lambda j, order, b=b: (order[b], j))
                for b in range(parts)
            ],
            out_specs=pl.BlockSpec((rows, block), lambda j, order: (0, j)),
        ),
        out_shape=jax.ShapeDtypeStruct((rows, cols), BF16),
        compiler_params=pltpu.CompilerParams(vmem_limit_bytes=VMEM_LIMIT),
    )(order, my, other, latent, gate, *([w_out] * parts))


def local(
    latent, context, conditions, mod_weight, norm_gain, w_query, w_key, w_value,
    query_gain, key_gain, lambdas, out_gain, w_out, *, n_sp, n_tp,
):
    tok_rows, _ = latent.shape
    heads_here = lambdas.shape[0]
    dk, dv = query_gain.shape[0], out_gain.shape[0]
    sp, tp = lax.axis_index("sp"), lax.axis_index("tp")
    chips = n_tp // 2

    def across(x):
        pieces = [x] + [
            lax.ppermute(x, "tp", [(i, (i + 2 * k) % n_tp) for i in range(n_tp)])
            for k in range(1, chips)
        ]
        return jnp.stack(pieces)

    def partner(x):
        return lax.ppermute(x, "tp", [(i, i ^ 1) for i in range(n_tp)])

    def shift(x, k):
        return lax.ppermute(x, "sp", [(i, (i + k) % n_sp) for i in range(n_sp)])

    places = jnp.arange(chips, dtype=jnp.int32)
    chip_order = (tp // 2 - places) % chips
    order = jnp.concatenate([2 * chip_order + tp % 2, 2 * chip_order + 1 - tp % 2])

    my_ctx = across(context)
    activated = jax.nn.silu(conditions).astype(BF16)
    modulation = jnp.stack(
        [
            jnp.sum(row[:, None, None] * mod_weight.astype(F32), axis=0)
            for row in activated.astype(F32)
        ]
    )
    if n_sp > 4:
        modulation = lax.psum(modulation, "sp")
    else:
        modulation = sum([shift(modulation, k) for k in range(1, n_sp)], modulation)
    gate = modulation[0, 2][None]
    packed = jnp.concatenate(
        [norm_gain[None], modulation[0, 1:2], modulation[0, 0:1],
         norm_gain[None], modulation[1, 1:2], modulation[1, 0:1]], axis=0
    )
    my_mods = across(packed)
    mods = jnp.concatenate([my_mods, partner(my_mods)])
    other_ctx = partner(my_ctx)

    pair = lambda g: jnp.concatenate([g, g])[None]
    ctx = project(
        order, my_ctx, other_ctx, mods[:, 3:], [w_key, w_value], [pair(key_gain)], (), dv
    )
    chunks = 2 if tok_rows % 16 == 0 else 1
    rows = tok_rows // chunks
    exchange = heads_here % n_sp == 0
    per = heads_here // n_sp if exchange else heads_here

    def swap(x):
        at = lambda k: lax.dynamic_slice_in_dim(x, (sp + k) % n_sp * per, per, 0)
        return [at(0)] + [shift(at(k), k) for k in range(1, n_sp)]

    lats = []
    for c in range(chunks):
        my = across(latent[c * rows : (c + 1) * rows])
        other = partner(my)
        positions = sp * tok_rows + c * rows + jnp.arange(rows, dtype=jnp.int32)
        lats.append(
            project(
                order, my, other, mods[:, :3], [w_query, w_key, w_value],
                [pair(query_gain), pair(key_gain)], tables(positions, dk), dv,
            )
        )
    gain = out_gain[None]
    if exchange:
        every_ctx = jnp.concatenate(swap(ctx), axis=1)
        every_lat = [jnp.concatenate(swap(x), axis=1) for x in lats]
        lam = lax.dynamic_slice_in_dim(lambdas, sp * per, per, 0)
        outs = []
        for c in range(chunks):
            seen = [(every_ctx, 0)] + [(x, 1) for x in every_lat[: c + 1]]
            rest = [(x, 1) for x in every_lat[c + 1 :]]
            before = tuple(outs[-1][-1:]) if outs else ()
            if rest:
                state = attend(lam, every_lat[c], 0, seen, gain, dv, final=False, after=before)
                outs.append([attend(lam, every_lat[c], 0, rest, gain, dv, state=state)])
                continue
            outs.append([])
            splits = 1
            for i in range(splits):
                out = attend(lam, every_lat[c], 0, seen, gain, dv, after=before, share=(i, splits))
                outs[-1].append(out)
                before = (out,)
    else:
        every_ctx = lax.all_gather(ctx, "sp", axis=1, tiled=True)
        lat = jnp.concatenate(lats, axis=1)
        every_lat = lax.all_gather(lat[:, :, dv:], "sp", axis=1, tiled=True)
        outs = [
            [attend(lambdas, x, 0, [(every_ctx, 0), (every_lat, 0)], gain, dv)] for x in lats
        ]
    head_out = []
    for out in outs:
        if exchange:
            split = n_sp // len(out)
            blocks = [
                out[k // split][:, k % split * rows : (k % split + 1) * rows] for k in range(n_sp)
            ]
            back = [shift(x, n_sp - k) if k else x for k, x in enumerate(blocks)]
            stacked = jnp.stack(back)
            ordered = [
                lax.dynamic_index_in_dim(stacked, (p - sp) % n_sp, 0, False)[h]
                for p in range(n_sp)
                for h in range(per)
            ]
        else:
            ordered = [out[0][h] for h in range(heads_here)]
        head_out.append(jnp.concatenate(ordered, axis=1))
    my_out = across(jnp.concatenate(head_out))
    return mix(order, my_out, partner(my_out), latent, gate, w_out)


def solution(mesh):
    in_specs = (
        P(("grp", "sp"), "tp"),
        P(("grp", "sp"), "tp"),
        P("grp", "sp"),
        P("sp", None, "tp"),
        P("tp"),
        P(None, "tp"),
        P(None, "tp"),
        P(None, "tp"),
        P(),
        P(),
        P("tp"),
        P(),
        P(None, "tp"),
    )

    def body(*args):
        return local(*args, n_sp=mesh.shape["sp"], n_tp=mesh.shape["tp"])

    return jax.shard_map(
        body, mesh=mesh, in_specs=in_specs, out_specs=P(("grp", "sp"), "tp"), check_vma=False
    )
```
